128 devices in a mesh: grp: 4 (over y, x), ep: 32 (over z, core).
Axes of the slice: x: 2, y: 2, z: 16, core: 2. Of those that a mesh axis runs over, the one named last changes fastest.
The devices are a block of a 8x8x16 slice.
Arguments:
- tokens: bfloat16 [4096, 2048], P(('grp', 'ep')), parts along dimension 0, may hold values from -6 to 6
- routes: int32 [4096, 8], P(('grp', 'ep')), parts along dimension 0, may hold values from 0 to 31, all different within a row; in each aligned block of 32 rows (0 to 31, 32 to 63, ...) at most 24 rows name the same one
- gates: float32 [4096, 8], P(('grp', 'ep')), parts along dimension 0, may hold values from 0.1 to 0.6
- norm_gain: float32 [2048], replicated, may hold values from 0.1 to 1.9
- expert_gate: bfloat16 [32, 2048, 512], P('ep'), may hold values from -0.125 to 0.125
- expert_up: bfloat16 [32, 2048, 512], P('ep'), may hold values from -0.125 to 0.125
- expert_down: bfloat16 [32, 512, 2048], P('ep'), may hold values from -0.25 to 0.25
- shared_gate: bfloat16 [2048, 512], replicated, may hold values from -0.125 to 0.125
- shared_up: bfloat16 [2048, 512], replicated, may hold values from -0.125 to 0.125
- shared_down: bfloat16 [512, 2048], replicated, may hold values from -0.25 to 0.25
Outputs:
- mixed: bfloat16 [4096, 2048], P(('grp', 'ep')), parts along dimension 0
The draws below stay inside these ranges and needn't reach their ends.
There are 4 independent parts, one for each index of `grp`. The reference program is written for one: setup_inputs(seed, part) draws one part's arguments, and reference() takes and returns one part's arrays. A program takes and returns all parts, laid end to end along the dimension named above; an argument that names none is the same for every part. Nothing has to cross between parts.
Inputs may be any that keep to these rules, and one draw needn't show every extreme that they name: `routes`: each row names 8 different experts; among the rows of one device no expert is named by more than 24 rows, a bound that some block reaches.
All inputs are finite; a program needn't handle non-finite values.
Results may differ from the reference program's by a relative error of at most 0.013.
Values may be sent and summed in bfloat16 or wider, within the bound.
A program may use at most 128 MiB of HBM per device.

```python
import math
import jax
import jax.numpy as jnp
import numpy as np
from jax import lax

D = 2048
DE = 512
TOPK = 8
TOK_DEV = 32
CAP = 24
EXPERTS = 32
TOKENS = 1024


def shard_levels(stream_key, shape, cuts, smallest, top_value):
    def one(dim, shards_of):
        draws = jax.random.uniform(jax.random.fold_in(jax.random.fold_in(stream_key, 6), dim), (shards_of,), jnp.float32, smallest / len(cuts), top_value / len(cuts))
        return jnp.repeat(jnp.exp(draws), shape[dim] // shards_of).reshape((-1,) + (1,) * (len(shape) - dim - 1))

    loudness = one(*cuts[0])
    for cut in cuts[1:]:
        loudness = loudness * one(*cut)
    return loudness


def assign_block(stream_key, own, number, rows, number_of, top, bound, lean):
    sequence = jax.random.permutation(stream_key, number_of)
    crowded, ordinary = shares(number_of, rows * top, bound, lean, True), shares(number_of, rows * top, bound, lean, False)
    places = jnp.arange(number_of)

    def named(tallies, offset_by):
        used = int((tallies > 0).sum())
        fixed = max(1, used // 4)
        moved = fixed + (places - fixed + offset_by * (used - fixed)) % max(1, number_of - fixed)
        return jnp.zeros((number_of,), jnp.int32).at[sequence[jnp.where(places < fixed, places, moved)]].set(jnp.asarray(tallies, jnp.int32))

    tallies = jnp.where(number % 4 == 0, named(crowded, number // 4), named(ordinary, number - number // 4 - 1))
    mixed = jax.random.permutation(jax.random.fold_in(own, 3), number_of)
    donor, taker = mixed[0:number_of // 2 * 2:2], mixed[1:number_of // 2 * 2:2]
    slack = jnp.minimum(tallies[donor] - 1, bound - tallies[taker]) // 2
    slack = jnp.where((donor == sequence[0]) | (taker == sequence[0]) | (tallies[taker] == 0), 0, jnp.maximum(slack, 0))
    moved = jax.random.randint(jax.random.fold_in(own, 4), (number_of // 2,), 0, 1 << 20) % (slack + 1)
    tallies = tallies.at[donor].add(-moved).at[taker].add(moved)
    items = jnp.searchsorted(jnp.cumsum(tallies), jnp.arange(rows * top), side="right").astype(jnp.int32)
    listing = items.reshape(top, rows).T
    listing = listing[jax.random.permutation(jax.random.fold_in(own, 1), rows)]
    offset_by = jax.random.randint(jax.random.fold_in(own, 2), (rows, 1), 0, top)
    return jnp.take_along_axis(listing, (jnp.arange(top)[None, :] + offset_by) % top, axis=1)


def shares(count, total, bound, skew, full):
    weights = [(1 << 20) // math.isqrt(rank ** skew) + 1 for rank in range(1, count + 1)]
    largest = bound if full else min(bound, max(-(-total // count), total * weights[0] // sum(weights)))
    least = 1 if total - largest >= count - 1 else 0
    holding, rest = [largest] + [least] * (count - 1), total - largest - least * (count - 1)
    while rest > 0:
        movable = [i for i in range(1, count) if holding[i] < largest] or [i for i in range(1, count) if holding[i] < bound]
        pool, remaining = sum([weights[i] for i in movable]), rest
        for i in movable:
            extra = min(bound - holding[i], max(1, remaining * weights[i] // pool), rest)
            holding[i] = holding[i] + extra
            rest = rest - extra
    return np.array(holding)


def normal_values(own_key, extent, spread, bound, pieces=(), kind=jnp.bfloat16):
    entries = spread * jax.random.normal(own_key, extent, jnp.float32)
    if pieces:
        entries = entries * shard_levels(own_key, extent, pieces, -0.22, 0.18)
    return jnp.clip(entries, -bound, bound).astype(kind)


def setup_inputs(seed: int = 0, part: int = 0) -> dict:
    arg_keys = jax.random.split(jax.random.key(seed), 11)
    own_keys = jax.random.split(jax.random.fold_in(arg_keys[10], part), 11)
    tokens = normal_values(own_keys[0], (TOKENS, D), 1.0, 6.0, ((0, 32),))
    routes_keys = jax.random.split(jax.random.fold_in(own_keys[1], 1), TOKENS // TOK_DEV)
    routes_turns = jax.random.permutation(jax.random.fold_in(own_keys[1], 3), TOKENS // TOK_DEV)
    routes = jax.vmap(lambda own, number: assign_block(jax.random.fold_in(own_keys[1], 2), own, number, TOK_DEV, EXPERTS, TOPK, CAP, 2))(routes_keys, routes_turns).reshape((TOKENS, TOPK))
    gates = jnp.clip(0.1 + 0.5 * jax.random.uniform(own_keys[2], (TOKENS, TOPK), jnp.float32) ** shard_levels(own_keys[2], (TOKENS, TOPK), ((0, 32),), -0.2, 0.2), 0.1, 0.6)
    norm_gain = jnp.clip(1.0 + 0.18 * jax.random.normal(arg_keys[3], (D,), jnp.float32), 0.1, 1.9)
    expert_gate = normal_values(arg_keys[4], (EXPERTS, D, DE), D ** -0.5, 0.125, ((0, 32),))
    expert_up = normal_values(arg_keys[5], (EXPERTS, D, DE), D ** -0.5, 0.125, ((0, 32),))
    expert_down = normal_values(arg_keys[6], (EXPERTS, DE, D), DE ** -0.5, 0.25, ((0, 32),))
    shared_gate = normal_values(arg_keys[7], (D, DE), D ** -0.5, 0.125)
    shared_up = normal_values(arg_keys[8], (D, DE), D ** -0.5, 0.125)
    shared_down = normal_values(arg_keys[9], (DE, D), DE ** -0.5, 0.25)
    return {"tokens": tokens, "routes": routes, "gates": gates, "norm_gain": norm_gain, "expert_gate": expert_gate, "expert_up": expert_up, "expert_down": expert_down, "shared_gate": shared_gate, "shared_up": shared_up, "shared_down": shared_down}


def norm_rows(tokens, norm_gain):
    values = tokens.astype(jnp.float32)
    scale = lax.rsqrt(lax.optimization_barrier(jnp.mean(values * values, axis=-1, keepdims=True)) + 1e-06)
    return (values * scale * norm_gain).astype(jnp.bfloat16)

def expert_rows(in_rows, w_gate, w_up, w_down):
    gate_pre = jnp.dot(in_rows, w_gate, preferred_element_type=jnp.float32)
    up_pre = jnp.dot(in_rows, w_up, preferred_element_type=jnp.float32)
    hidden = (jax.nn.silu(gate_pre) * up_pre).astype(jnp.bfloat16)
    return jnp.dot(hidden, w_down, preferred_element_type=jnp.float32).astype(jnp.bfloat16)

def reference(tokens, routes, gates, norm_gain, expert_gate, expert_up, expert_down, shared_gate, shared_up, shared_down):
    normed = norm_rows(tokens, norm_gain)
    chosen = lax.optimization_barrier(jnp.sum(jax.nn.one_hot(routes, EXPERTS, dtype=jnp.float32) * gates[:, :, None], axis=1))

    def one_expert(carry, packed):
        w_gate, w_up, w_down, weight = packed
        answer = expert_rows(normed, w_gate, w_up, w_down)
        return (carry + weight[:, None] * answer.astype(jnp.float32), None)
    start = jnp.zeros((normed.shape[0], normed.shape[1]), jnp.float32)
    routed, _ = lax.scan(one_expert, start, (expert_gate, expert_up, expert_down, chosen.T))
    gate_pre = jnp.dot(normed, shared_gate, preferred_element_type=jnp.float32)
    up_pre = jnp.dot(normed, shared_up, preferred_element_type=jnp.float32)
    shared_hidden = (jax.nn.silu(gate_pre) * up_pre).astype(jnp.bfloat16)
    shared = jnp.dot(shared_hidden, shared_down, preferred_element_type=jnp.float32)
    return (routed + shared).astype(jnp.bfloat16)
```

```python
import functools

import jax
import jax.numpy as jnp
from jax import lax
from jax.experimental import pallas as pl
from jax.experimental.pallas import tpu as pltpu
from jax.sharding import PartitionSpec as P

MESH = pl.DeviceIdType.MESH
ROW_CUTS = 2
COL_CUTS = 2
LANES = 128


def layer_kernel(
    half,
    tokens_ref,
    routes_ref,
    gates_ref,
    gain_ref,
    e_gate,
    e_up,
    e_down,
    s_gate,
    s_up,
    s_down,
    out_ref,
    blocks,
    tiles,
    w_gate,
    w_up,
    w_down,
    v_gate,
    v_up,
    v_down,
    hidden,
    kept,
    given,
    taken,
    partial,
    final,
    shared,
    weight_sem,
    ring_send,
    ring_recv,
    pair_send,
    pair_recv,
    tile_send,
    tile_recv,
    tpair_send,
    tpair_recv,
    give_send,
    give_recv,
    sum_send,
    sum_recv,
    final_recv,
):
    rows, width = tokens_ref.shape
    inner = w_down.shape[0]
    chips = 2 * half
    me = lax.axis_index("ep")
    place, core = me // 2, lax.rem(me, 2)
    step_by = 1 - 2 * core
    ahead = lax.rem(place + step_by + chips, chips)
    behind = lax.rem(place - step_by + chips, chips)
    following = {"ep": ahead * 2 + core}
    previous = {"ep": behind * 2 + core}
    partner = {"ep": place * 2 + 1 - core}
    crossing = {"ep": ahead * 2 + 1 - core}

    loads = [
        pltpu.make_async_copy(e_gate.at[0], w_gate, weight_sem.at[0]),
        pltpu.make_async_copy(e_up.at[0], w_up, weight_sem.at[1]),
        pltpu.make_async_copy(e_down.at[0], w_down, weight_sem.at[2]),
        pltpu.make_async_copy(s_gate, v_gate, weight_sem.at[3]),
        pltpu.make_async_copy(s_up, v_up, weight_sem.at[4]),
        pltpu.make_async_copy(s_down, v_down, weight_sem.at[5]),
    ]
    barrier = pltpu.get_barrier_semaphore()
    for other in (previous, partner, crossing):
        pl.semaphore_signal(barrier, inc=1, device_id=other, device_id_type=MESH)
    for load in loads:
        load.start()

    values = tokens_ref[...].astype(jnp.float32)
    scale = lax.rsqrt(jnp.mean(values * values, axis=-1, keepdims=True) + 1e-06)
    blocks[0, 0:rows, :] = (values * scale * gain_ref[...]).astype(jnp.bfloat16)

    groups = rows // 8
    experts = LANES // groups
    lane = lax.broadcasted_iota(jnp.int32, (8, LANES), 1)
    tile = jnp.zeros((8, LANES), jnp.float32)
    for group in range(groups):
        for pick in range(routes_ref.shape[1]):
            where = routes_ref[group * 8:group * 8 + 8, pick:pick + 1] + group * experts
            gate = gates_ref[group * 8:group * 8 + 8, pick:pick + 1]
            tile += jnp.where(lane == where, gate, 0.0)
    tiles[0, 0] = tile

    pl.semaphore_wait(barrier, 3)

    cut_rows, cut_cols = rows // ROW_CUTS, width // COL_CUTS
    cuts = [(r * cut_rows, c * cut_cols) for r in range(ROW_CUTS) for c in range(COL_CUTS)]
    ncuts = len(cuts)

    def area(ref, at, first, cut):
        r, c = cuts[cut]
        return ref.at[at, pl.ds(first + r, cut_rows), pl.ds(c, cut_cols)]

    def remote(src, dst, send, recv, device):
        return pltpu.make_async_remote_copy(
            src_ref=src, dst_ref=dst, send_sem=send, recv_sem=recv, device_id=device, device_id_type=MESH
        )

    def ring(s, b, q):
        return remote(
            area(blocks, s, b * rows, q), area(blocks, s + 1, b * rows, q),
            ring_send.at[s, b, q], ring_recv.at[s + 1, b, q], following,
        )

    def pair(s, b, q, first):
        return remote(
            area(blocks, s, b * rows, q), area(blocks, s, first, q),
            pair_send.at[s, b, q], pair_recv.at[s, b, q], partner,
        )

    def tile_ring(s, count):
        return remote(
            tiles.at[s, pl.ds(0, count)], tiles.at[s + 1, pl.ds(0, count)],
            tile_send.at[s], tile_recv.at[s + 1], following,
        )

    def tile_pair(s, count, first):
        return remote(
            tiles.at[s, pl.ds(0, count)], tiles.at[s, pl.ds(first, count)],
            tpair_send.at[s], tpair_recv.at[s], partner,
        )

    def give(s, first, count):
        return remote(
            given.at[s, pl.ds(first, count)], taken.at[s, pl.ds(first, count)],
            give_send.at[s], give_recv.at[s], partner,
        )

    row_id = lax.broadcasted_iota(jnp.int32, (rows, LANES), 0)
    lane_id = lax.broadcasted_iota(jnp.int32, (rows, LANES), 1)
    own_lane = (row_id // 8) * experts + me

    def columns_of(s, count):
        cols = []
        for b in range(count):
            tile = tiles[s, b]
            full = jnp.concatenate([tile] * groups, axis=0)
            cols.append(jnp.sum(jnp.where(lane_id == own_lane, full, 0.0), axis=1, keepdims=True))
        return jnp.concatenate(cols, axis=0)

    up_step = inner // 2
    down_step = width // 2

    def up_piece(s, count, i):
        x = blocks[s, 0:count * rows, :]
        cols = slice(i * up_step, (i + 1) * up_step)
        gate_pre = jnp.dot(x, w_gate[:, cols], preferred_element_type=jnp.float32)
        up_pre = jnp.dot(x, w_up[:, cols], preferred_element_type=jnp.float32)
        act = gate_pre * jax.nn.sigmoid(gate_pre) * up_pre
        hidden[0:count * rows, cols] = (act * columns_of(s, count)).astype(jnp.bfloat16)

    def down_piece(s, count, i, layout):
        cols = slice(i * down_step, (i + 1) * down_step)
        answer = jnp.dot(hidden[0:count * rows, :], w_down[:, cols], preferred_element_type=jnp.float32)
        for dst, dst_row, src_row, n in layout:
            dst[s, dst_row:dst_row + n, cols] = answer[src_row:src_row + n].astype(dst.dtype)

    middle = ((given, 0, 0, 2 * rows), (kept, 0, 2 * rows, 2 * rows))
    first = ((kept, 0, 0, rows), (given, 0, rows, rows))
    last = ((kept, rows, 0, rows), (given, rows, rows, rows))

    def pieces_of(s, count, layout):
        return [
            lambda: up_piece(s, count, 0),
            lambda: up_piece(s, count, 1),
            lambda: down_piece(s, count, 0, layout),
            lambda: down_piece(s, count, 1, layout),
        ]

    for q in range(ncuts):
        ring(0, 0, q).start()
        pair(0, 0, q, rows).start()
    tile_pair(0, 1, 1).start()
    for q in range(ncuts):
        pair(0, 0, q, rows).wait_recv()
        ring(0, 1, q).start()
    tile_pair(0, 1, 1).wait_recv()
    tile_ring(0, 2).start()
    for load in loads[:3]:
        load.wait()

    def arrivals(s, pieces):
        todo = list(pieces)
        for b in range(2):
            for q in range(ncuts):
                ring(s - 1, b, q).wait_recv()
                if isinstance(s, int) and s == half - 1:
                    if b == 0:
                        ring(s, b, q).start()
                else:
                    ring(s, b, q).start()
                pair(s, b, q, (2 + b) * rows).start()
                if b == 1 and q == ncuts - 1:
                    tile_ring(s - 1, 2).wait_recv()
                    tile_ring(s, 1 if isinstance(s, int) and s == half - 1 else 2).start()
                    tile_pair(s, 2, 2).start()
                left = 2 * ncuts - (b * ncuts + q)
                run = -(-len(todo) // left)
                for piece in todo[:run]:
                    piece()
                todo = todo[run:]

    def ready(s):
        for b in range(2):
            for q in range(ncuts):
                pair(s, b, q, (2 + b) * rows).wait_recv()
        tile_pair(s, 2, 2).wait_recv()

    arrivals(1, pieces_of(0, 2, first))
    give(0, 0, rows).start()

    def body(s, carry):
        ready(s - 1)
        arrivals(s, pieces_of(s - 1, 4, middle))
        give(s - 1, 0, 2 * rows).start()
        return carry

    lax.fori_loop(2, half - 1, body, 0)
    ready(half - 2)
    arrivals(half - 1, pieces_of(half - 2, 4, middle))
    give(half - 2, 0, 2 * rows).start()

    ready(half - 1)
    todo = pieces_of(half - 1, 4, middle)
    for q in range(ncuts):
        ring(half - 1, 0, q).wait_recv()
        pair(half, 0, q, rows).start()
        if q == ncuts - 1:
            tile_ring(half - 1, 1).wait_recv()
            tile_pair(half, 1, 1).start()
        todo[q]()
    for piece in todo[ncuts:]:
        piece()
    give(half - 1, 0, 2 * rows).start()
    for q in range(ncuts):
        pair(half, 0, q, rows).wait_recv()
    tile_pair(half, 1, 1).wait_recv()
    for piece in pieces_of(half, 2, last):
        piece()
    give(half, rows, rows).start()

    def send_sum(k, b, q):
        if isinstance(k, int) and k == 1:
            return remote(
                area(partial, k, b * rows, q), area(final, 1 - b, 0, q),
                sum_send.at[k, b, q], final_recv.at[1 - b, q], crossing if b == 0 else following,
            )
        return remote(
            area(partial, k, b * rows, q), area(partial, k - 1, b * rows, q),
            sum_send.at[k, b, q], sum_recv.at[k - 1, b, q], following,
        )

    def came(k, b, q):
        return remote(
            area(partial, k, b * rows, q), area(partial, k, b * rows, q),
            sum_send.at[k, b, q], sum_recv.at[k, b, q], following,
        )

    def add_up(k, b, incoming):
        for q in range(ncuts):
            r, c = cuts[q]
            at = (k, pl.ds(b * rows + r, cut_rows), pl.ds(c, cut_cols))
            total = kept[at] + taken[at].astype(jnp.float32)
            if incoming:
                came(k, b, q).wait_recv()
                total += partial[at].astype(jnp.float32)
            partial[at] = total.astype(jnp.bfloat16)
            send_sum(k, b, q).start()

    give(half - 1, 0, 2 * rows).wait_recv()
    add_up(half - 1, 0, False)
    give(half, rows, rows).wait_recv()
    add_up(half, 1, False)

    for load in loads[3:]:
        load.wait()
    x = blocks[0, 0:rows, :]
    gate_pre = jnp.dot(x, v_gate[...], preferred_element_type=jnp.float32)
    up_pre = jnp.dot(x, v_up[...], preferred_element_type=jnp.float32)
    act = (gate_pre * jax.nn.sigmoid(gate_pre) * up_pre).astype(jnp.bfloat16)
    shared[...] = jnp.dot(act, v_down[...], preferred_element_type=jnp.float32)

    def sums(j, carry):
        give(half - 1 - j, 0, 2 * rows).wait_recv()
        add_up(half - 1 - j, 0, True)
        add_up(half - j, 1, True)
        return carry

    lax.fori_loop(1, half - 2, sums, 0)
    give(1, 0, 2 * rows).wait_recv()
    add_up(1, 0, True)
    add_up(2, 1, True)
    add_up(1, 1, True)

    give(0, 0, rows).wait_recv()
    shared[...] += kept[0, 0:rows, :] + taken[0, 0:rows, :].astype(jnp.float32)
    for q in range(ncuts):
        r, c = cuts[q]
        for i in (1, 0):
            remote(
                area(final, i, 0, q), area(final, i, 0, q), sum_send.at[1, i, q], final_recv.at[i, q], following
            ).wait_recv()
        at = (pl.ds(r, cut_rows), pl.ds(c, cut_cols))
        total = shared[at]
        for i in range(2):
            total += final[(i,) + at].astype(jnp.float32)
        out_ref[at] = total.astype(jnp.bfloat16)

    def sent_blocks(s, carry):
        for b in range(2):
            for q in range(ncuts):
                ring(s, b, q).wait_send()
        tile_ring(s, 2).wait_send()
        return carry

    def sent_pairs(s, carry):
        for b in range(2):
            for q in range(ncuts):
                pair(s, b, q, (2 + b) * rows).wait_send()
        tile_pair(s, 2, 2).wait_send()
        give(s, 0, 2 * rows).wait_send()
        return carry

    def sent_sums(k, carry):
        for b in range(2):
            for q in range(ncuts):
                came(k, b, q).wait_send()
        return carry

    lax.fori_loop(0, half - 1, sent_blocks, 0)
    lax.fori_loop(1, half, sent_pairs, 0)
    lax.fori_loop(1, half, sent_sums, 0)
    for q in range(ncuts):
        ring(half - 1, 0, q).wait_send()
        pair(0, 0, q, rows).wait_send()
        pair(half, 0, q, rows).wait_send()
        came(half, 1, q).wait_send()
    tile_ring(half - 1, 1).wait_send()
    tile_pair(0, 1, 1).wait_send()
    tile_pair(half, 1, 1).wait_send()
    give(0, 0, rows).wait_send()
    give(half, rows, rows).wait_send()


def local(tokens, routes, gates, norm_gain, e_gate, e_up, e_down, s_gate, s_up, s_down):
    rows, width = tokens.shape
    inner = e_down.shape[1]
    half = lax.axis_size("ep") // 4
    steps = half + 1
    ncuts = ROW_CUTS * COL_CUTS
    bf16, f32 = jnp.bfloat16, jnp.float32
    dma = pltpu.SemaphoreType.DMA
    whole = pl.BlockSpec(memory_space=pltpu.VMEM)
    apart = pl.BlockSpec(memory_space=pl.ANY)
    return pl.pallas_call(
        functools.partial(layer_kernel, half),
        out_shape=jax.ShapeDtypeStruct((rows, width), bf16),
        in_specs=[whole] * 4 + [apart] * 6,
        out_specs=whole,
        scratch_shapes=[
            pltpu.VMEM((steps, 4 * rows, width), bf16),
            pltpu.VMEM((steps, 4, 8, LANES), f32),
            pltpu.VMEM((width, inner), bf16),
            pltpu.VMEM((width, inner), bf16),
            pltpu.VMEM((inner, width), bf16),
            pltpu.VMEM((width, inner), bf16),
            pltpu.VMEM((width, inner), bf16),
            pltpu.VMEM((inner, width), bf16),
            pltpu.VMEM((4 * rows, inner), bf16),
            pltpu.VMEM((steps, 2 * rows, width), f32),
            pltpu.VMEM((steps, 2 * rows, width), bf16),
            pltpu.VMEM((steps, 2 * rows, width), bf16),
            pltpu.VMEM((steps, 2 * rows, width), bf16),
            pltpu.VMEM((2, rows, width), bf16),
            pltpu.VMEM((rows, width), f32),
            dma((6,)),
            dma((steps, 2, ncuts)),
            dma((steps, 2, ncuts)),
            dma((steps, 2, ncuts)),
            dma((steps, 2, ncuts)),
            dma((steps,)),
            dma((steps,)),
            dma((steps,)),
            dma((steps,)),
            dma((steps,)),
            dma((steps,)),
            dma((steps, 2, ncuts)),
            dma((steps, 2, ncuts)),
            dma((2, ncuts)),
        ],
        compiler_params=pltpu.CompilerParams(
            collective_id=0, has_side_effects=True, vmem_limit_bytes=60 << 20
        ),
    )(tokens, routes, gates, norm_gain.reshape(1, width), e_gate, e_up, e_down, s_gate, s_up, s_down)


def solution(mesh):
    token_spec = P(("grp", "ep"), None)
    expert_spec = P("ep", None, None)
    return jax.shard_map(
        local,
        mesh=mesh,
        in_specs=(token_spec, token_spec, token_spec, P(), expert_spec, expert_spec, expert_spec, P(), P(), P()),
        out_specs=token_spec,
        check_vma=False,
    )
```
